32 devices in a mesh: sp: 8 (over z, y), dp: 4 (over x, core).
Axes of the slice: x: 2, y: 2, z: 4, core: 2. Of those that a mesh axis runs over, the one named last changes fastest.
Arguments:
- query_nope: bfloat16 [4, 2048, 16, 128], P('dp', 'sp'), may hold values from -6 to 6
- query_rope: bfloat16 [4, 2048, 16, 64], P('dp', 'sp'), may hold values from -160 to 160
- latent: bfloat16 [4, 2048, 256], P('dp', 'sp'), may hold values from -6 to 6
- key_rope: bfloat16 [4, 2048, 64], P('dp', 'sp'), may hold values from -4 to 4
- resid: bfloat16 [4, 2048, 2048], P('dp', 'sp'), may hold values from -6 to 6
- latent_gain: float32 [256], replicated, may hold values from 0.1 to 1.9
- key_up: bfloat16 [256, 2048], P(None, 'sp'), may hold values from -0.375 to 0.375
- value_up: bfloat16 [256, 2048], P(None, 'sp'), may hold values from -0.375 to 0.375
- out_proj: bfloat16 [2048, 2048], P('sp', 'dp'), may hold values from -0.125 to 0.125
- norm_gain: float32 [2048], replicated, may hold values from 0.1 to 1.9
- expert_gate: bfloat16 [8, 2048, 1024], P('sp'), may hold values from -0.125 to 0.125
- expert_up: bfloat16 [8, 2048, 1024], P('sp'), may hold values from -0.125 to 0.125
- expert_down: bfloat16 [8, 1024, 2048], P('sp'), may hold values from -0.1875 to 0.1875
- routes: int32 [4, 2048, 2], P('dp', 'sp'), may hold values from 0 to 7, all different within a row; in each aligned block of 256 rows (0 to 255, 256 to 511, ..., all dimensions but the last counted through in order) at most 128 rows name the same one
- route_weight: float32 [4, 2048, 2], P('dp', 'sp'), may hold values from 0.2 to 1
Outputs:
- mixed: bfloat16 [4, 2048, 2048], P('dp', 'sp')
The draws below stay inside these ranges and needn't reach their ends.
Inputs may be any that keep to these rules, and one draw needn't show every extreme that they name: `routes`: each token names two different experts. Among the tokens of one device no expert is named more than 128 times, and in every draw some expert is named exactly 128 times by some device's tokens.
All inputs are finite; a program needn't handle non-finite values.
Results may differ from the reference program's by a relative error of at most 0.0075.
Values may be sent and summed in bfloat16 or wider, within the bound.
A program may use at most 128 MiB of HBM per device.

```python
import math
import jax
import jax.numpy as jnp
import numpy as np
from jax import lax

D = 2048
HEADS = 16
NOPE = 128
ROPE = 64
VDIM = 128
LATENT = 256
FFE = 1024
TOK_DEV = 256
LENGTH = 2048
SEQS = 4
EXPERTS = 8
CAP = 128
N_SP = 8
N_DP = 4


def rope_pair(key):
    base_key = jax.random.fold_in(key, 911)
    key_draw, query_draw = jax.random.split(base_key, 2)
    keys_raw = jnp.clip(jax.random.normal(key_draw, (SEQS, LENGTH, ROPE), jnp.float32), -4.0, 4.0)
    queries = jnp.clip(jax.random.normal(query_draw, (SEQS, LENGTH, HEADS, ROPE), jnp.float32), -4.0, 4.0)
    return (queries, keys_raw)


def draw_query_rope(key, part):
    return rope_pair(key)[0].astype(jnp.bfloat16)


def draw_key_rope(key, part):
    return rope_pair(key)[1].astype(jnp.bfloat16)


def steps_of(rng, extent, cuts, low, top_value):
    def one(axis_at, parts):
        steps = jax.random.uniform(jax.random.fold_in(jax.random.fold_in(rng, 6), axis_at), (parts,), jnp.float32, low / len(cuts), top_value / len(cuts))
        return jnp.repeat(jnp.exp(steps), extent[axis_at] // parts).reshape((-1,) + (1,) * (len(extent) - axis_at - 1))

    factor_of = one(*cuts[0])
    for cut in cuts[1:]:
        factor_of = factor_of * one(*cut)
    return factor_of


def deal_out(key, own, number, rows, count, top, most, lean):
    order = jax.random.permutation(key, count)
    heavy_load, usual = load_shares(count, rows * top, most, lean, True), load_shares(count, rows * top, most, lean, False)
    places = jnp.arange(count)

    def named(tallies, offset_by):
        used = int((tallies > 0).sum())
        fixed = max(1, used // 4)
        shifted = fixed + (places - fixed + offset_by * (used - fixed)) % max(1, count - fixed)
        return jnp.zeros((count,), jnp.int32).at[order[jnp.where(places < fixed, places, shifted)]].set(jnp.asarray(tallies, jnp.int32))

    tallies = jnp.where(number % 4 == 0, named(heavy_load, number // 4), named(usual, number - number // 4 - 1))
    mixed = jax.random.permutation(jax.random.fold_in(own, 3), count)
    giver, receiver = mixed[0:count // 2 * 2:2], mixed[1:count // 2 * 2:2]
    slack = jnp.minimum(tallies[giver] - 1, most - tallies[receiver]) // 2
    slack = jnp.where((giver == order[0]) | (receiver == order[0]) | (tallies[receiver] == 0), 0, jnp.maximum(slack, 0))
    shifted = jax.random.randint(jax.random.fold_in(own, 4), (count // 2,), 0, 1 << 20) % (slack + 1)
    tallies = tallies.at[giver].add(-shifted).at[receiver].add(shifted)
    items = jnp.searchsorted(jnp.cumsum(tallies), jnp.arange(rows * top), side="right").astype(jnp.int32)
    listing = items.reshape(top, rows).T
    listing = listing[jax.random.permutation(jax.random.fold_in(own, 1), rows)]
    offset_by = jax.random.randint(jax.random.fold_in(own, 2), (rows, 1), 0, top)
    return jnp.take_along_axis(listing, (jnp.arange(top)[None, :] + offset_by) % top, axis=1)


def load_shares(number_of, total, limit, slope, full):
    portions = [(1 << 20) // math.isqrt(standing ** slope) + 1 for standing in range(1, number_of + 1)]
    largest = limit if full else min(limit, max(-(-total // number_of), total * portions[0] // sum(portions)))
    least = 1 if total - largest >= number_of - 1 else 0
    counts, rest = [largest] + [least] * (number_of - 1), total - largest - least * (number_of - 1)
    while rest > 0:
        candidates = [i for i in range(1, number_of) if counts[i] < largest] or [i for i in range(1, number_of) if counts[i] < limit]
        mass, remaining = sum([portions[i] for i in candidates]), rest
        for i in candidates:
            more = min(limit - counts[i], max(1, remaining * portions[i] // mass), rest)
            counts[i] = counts[i] + more
            rest = rest - more
    return np.array(counts)


def centred(key, shape, deviation, reach, cuts=(), held_as=jnp.bfloat16):
    drawn = jax.random.normal(key, shape, jnp.float32) * deviation
    if len(cuts) > 0:
        drawn = steps_of(key, shape, cuts, -0.22, 0.18) * drawn
    return jnp.clip(drawn, min=-reach, max=reach).astype(held_as)


def setup_inputs(seed: int = 0) -> dict:
    keys = jax.random.split(jax.random.key(seed), 16)
    query_nope = centred(keys[0], (SEQS, LENGTH, HEADS, NOPE), 1.0, 6.0, ((0, 4), (1, 8)))
    query_rope = draw_query_rope(jax.random.fold_in(keys[15], 71), 0)
    latent = centred(keys[2], (SEQS, LENGTH, LATENT), 1.0, 6.0, ((0, 4), (1, 8)))
    key_rope = draw_key_rope(jax.random.fold_in(keys[15], 71), 0)
    resid = centred(keys[4], (SEQS, LENGTH, D), 1.0, 6.0, ((0, 4), (1, 8)))
    latent_gain = jnp.clip(1.0 + 0.18 * jax.random.normal(keys[5], (LATENT,), jnp.float32), 0.1, 1.9)
    key_up = centred(keys[6], (LATENT, HEADS * NOPE), LATENT ** -0.5, 0.375, ((1, 8),))
    value_up = centred(keys[7], (LATENT, HEADS * VDIM), LATENT ** -0.5, 0.375, ((1, 8),))
    out_proj = centred(keys[8], (HEADS * VDIM, D), (HEADS * VDIM) ** -0.5, 0.125, ((0, 8), (1, 4)))
    norm_gain = jnp.clip(1.0 + 0.18 * jax.random.normal(keys[9], (D,), jnp.float32), 0.1, 1.9)
    expert_gate = centred(keys[10], (EXPERTS, D, FFE), D ** -0.5, 0.125, ((0, 8),))
    expert_up = centred(keys[11], (EXPERTS, D, FFE), D ** -0.5, 0.125, ((0, 8),))
    expert_down = centred(keys[12], (EXPERTS, FFE, D), FFE ** -0.5, 0.1875, ((0, 8),))
    routes_keys = jax.random.split(jax.random.fold_in(keys[13], 1), SEQS * LENGTH // TOK_DEV)
    routes_turns = jax.random.permutation(jax.random.fold_in(keys[13], 3), SEQS * LENGTH // TOK_DEV)
    routes = jax.vmap(lambda own, number: deal_out(jax.random.fold_in(keys[13], 2), own, number, TOK_DEV, EXPERTS, 2, CAP, 1))(routes_keys, routes_turns).reshape((SEQS, LENGTH, 2))
    route_weight = jnp.clip(0.2 + 0.8 * jax.random.uniform(keys[14], (SEQS, LENGTH, 2), jnp.float32) ** steps_of(keys[14], (SEQS, LENGTH, 2), ((0, 4), (1, 8)), -0.2, 0.2), 0.2, 1.0)
    return dict(query_nope=query_nope, query_rope=query_rope, latent=latent, key_rope=key_rope, resid=resid, latent_gain=latent_gain, key_up=key_up, value_up=value_up, out_proj=out_proj, norm_gain=norm_gain, expert_gate=expert_gate, expert_up=expert_up, expert_down=expert_down, routes=routes, route_weight=route_weight)


epsilon = 1e-06
rope_base = 10000.0
masked_score = -1e+30

def rotate(values, positions):
    half_width = values.shape[-1] // 2
    frequency = rope_base ** (-jnp.arange(half_width, dtype=jnp.float32) / half_width)
    angles = positions.astype(jnp.float32)[:, None] * frequency[None, :]
    cosine = jnp.cos(angles)
    sine_part = jnp.sin(angles)
    if values.ndim == 3:
        cosine = cosine[:, None, :]
        sine_part = sine_part[:, None, :]
    floats = values.astype(jnp.float32)
    first_half = floats[..., :half_width]
    second_half = floats[..., half_width:]
    turned = jnp.concatenate([first_half * cosine - second_half * sine_part, second_half * cosine + first_half * sine_part], axis=-1)
    return turned.astype(jnp.bfloat16)

def rms_scaled(values, gain):
    floats = values.astype(jnp.float32)
    return floats * lax.rsqrt(lax.optimization_barrier(jnp.mean(floats * floats, axis=-1, keepdims=True)) + epsilon) * gain

def assign_slots(route_block, experts_all, capacity):
    flat_routes = route_block.reshape(-1)
    onehot = (flat_routes[:, None] == jnp.arange(experts_all, dtype=jnp.int32)[None, :]).astype(jnp.int32)
    earlier = jnp.cumsum(onehot, axis=0) - onehot
    placed = lax.optimization_barrier(jnp.sum(earlier * onehot, axis=1))
    return (flat_routes * capacity + placed).astype(jnp.int32)

def fill_slots(rows, slot_ids, experts_all, capacity):
    pairs = slot_ids.shape[0]
    matches = jnp.arange(experts_all * capacity, dtype=jnp.int32)[:, None] == slot_ids[None, :]
    source = lax.optimization_barrier(jnp.sum(jnp.where(matches, jnp.arange(pairs, dtype=jnp.int32)[None, :], 0), axis=1)) // 2
    filled = jnp.any(matches, axis=1)
    picked = jnp.take(rows, source.astype(jnp.int32), axis=0)
    chosen = jnp.where(filled[:, None], picked, jnp.zeros_like(picked))
    return chosen.reshape(experts_all, capacity, rows.shape[-1])

def combine_slots(returned, slot_ids, weights):
    flat_back = returned.reshape(-1, returned.shape[-1])
    picked = jnp.take(flat_back, slot_ids, axis=0).astype(jnp.float32).reshape(weights.shape[0], 2, -1)
    return lax.optimization_barrier(jnp.sum(weights[:, :, None] * picked, axis=1))

def expert_rows(rows, gate_weight, up_weight, down_weight):
    gate = jnp.dot(rows, gate_weight, preferred_element_type=jnp.float32)
    upward = jnp.dot(rows, up_weight, preferred_element_type=jnp.float32)
    hidden = (jax.nn.silu(gate) * upward).astype(jnp.bfloat16)
    return jnp.dot(hidden, down_weight, preferred_element_type=jnp.float32).astype(jnp.bfloat16)

def head_attention(query_plain, query_turn, key_plain, key_turn, value_head, block):
    length = key_plain.shape[0]
    blocks = length // block
    scale = (query_plain.shape[-1] + query_turn.shape[-1]) ** (-0.5)
    key_ids = jnp.arange(length, dtype=jnp.int32)

    def one_block(items):
        index, plain_block, turn_block = items
        scores = jnp.dot(plain_block, key_plain.T, preferred_element_type=jnp.float32)
        scores = (scores + jnp.dot(turn_block, key_turn.T, preferred_element_type=jnp.float32)) * scale
        row_ids = index * block + jnp.arange(block, dtype=jnp.int32)
        allowed = key_ids[None, :] <= row_ids[:, None]
        scores = jnp.where(allowed, scores, masked_score)
        largest = lax.optimization_barrier(jnp.max(scores, axis=-1, keepdims=True))
        powers = jnp.exp(scores - largest)
        attend = (powers / lax.optimization_barrier(jnp.sum(powers, axis=-1, keepdims=True))).astype(jnp.bfloat16)
        return jnp.dot(attend, value_head, preferred_element_type=jnp.float32).astype(jnp.bfloat16)
    result = lax.map(one_block, (jnp.arange(blocks, dtype=jnp.int32), query_plain.reshape(blocks, block, -1), query_turn.reshape(blocks, block, -1)))
    return result.reshape(length, -1)

def reference(query_nope, query_rope, latent, key_rope, resid, latent_gain, key_up, value_up, out_proj, norm_gain, expert_gate, expert_up, expert_down, routes, route_weight):
    positions = jnp.arange(LENGTH, dtype=jnp.int32)
    block = min(512, LENGTH)
    key_turned = jax.vmap(lambda item: rotate(item, positions))(key_rope)
    query_turned = jax.vmap(lambda item: rotate(item, positions))(query_rope)
    latent_normed = rms_scaled(latent, latent_gain).astype(jnp.bfloat16)
    flat_latent = latent_normed.reshape(-1, LATENT)
    key_nope = jnp.dot(flat_latent, key_up, preferred_element_type=jnp.float32).astype(jnp.bfloat16).reshape(SEQS, LENGTH, HEADS, NOPE)
    values = jnp.dot(flat_latent, value_up, preferred_element_type=jnp.float32).astype(jnp.bfloat16).reshape(SEQS, LENGTH, HEADS, VDIM)

    def one_sequence(items):
        plain_heads, turn_heads, key_heads, value_heads, key_turn = items
        return lax.map(lambda head: head_attention(head[0], head[1], head[2], key_turn, head[3], block), (plain_heads, turn_heads, key_heads, value_heads))
    heads_out = lax.map(one_sequence, (jnp.transpose(query_nope, (0, 2, 1, 3)), jnp.transpose(query_turned, (0, 2, 1, 3)), jnp.transpose(key_nope, (0, 2, 1, 3)), jnp.transpose(values, (0, 2, 1, 3)), key_turned))
    heads_out = jnp.transpose(heads_out, (0, 2, 1, 3)).reshape(SEQS * LENGTH, HEADS * VDIM)
    projected = jnp.dot(heads_out, out_proj, preferred_element_type=jnp.float32).astype(jnp.bfloat16)
    after_attention = resid.reshape(-1, D).astype(jnp.float32) + projected.astype(jnp.float32)
    normed = rms_scaled(after_attention, norm_gain).astype(jnp.bfloat16)
    normed_blocks = normed.reshape(N_DP, N_SP, TOK_DEV, D)
    route_blocks = routes.reshape(N_DP, N_SP, TOK_DEV, 2)
    slot_ids = jax.vmap(jax.vmap(lambda item: assign_slots(item, EXPERTS, CAP)))(route_blocks)
    buffers = jax.vmap(jax.vmap(lambda rows, ids: fill_slots(rows, ids, EXPERTS, CAP)))(normed_blocks, slot_ids)
    by_expert = jnp.transpose(buffers, (2, 0, 1, 3, 4)).reshape(EXPERTS, N_DP * N_SP * CAP, D)
    outputs = lax.map(lambda item: expert_rows(item[0], item[1], item[2], item[3]), (by_expert, expert_gate, expert_up, expert_down))
    returned = jnp.transpose(outputs.reshape(EXPERTS, N_DP, N_SP, CAP, D), (1, 2, 0, 3, 4))
    routed = jax.vmap(jax.vmap(combine_slots))(returned, slot_ids, route_weight.reshape(N_DP, N_SP, TOK_DEV, 2))
    mixed = after_attention + routed.reshape(-1, D)
    return mixed.astype(jnp.bfloat16).reshape(SEQS, LENGTH, D)
```

```python
import functools

import jax
import jax.numpy as jnp
from jax import lax
from jax.experimental import pallas as pl
from jax.experimental.pallas import tpu as pltpu
from jax.sharding import PartitionSpec as P

epsilon = 1e-06
rope_base = 10000.0
masked_score = -1e30
log2_e = 1.4426950408889634


def rotate(values, positions):
    half_width = values.shape[-1] // 2
    frequency = rope_base ** (-jnp.arange(half_width, dtype=jnp.float32) / half_width)
    angles = positions.astype(jnp.float32)[:, None] * frequency[None, :]
    cosine = jnp.cos(angles)
    sine_part = jnp.sin(angles)
    if values.ndim == 3:
        cosine = cosine[:, None, :]
        sine_part = sine_part[:, None, :]
    floats = values.astype(jnp.float32)
    first_half = floats[..., :half_width]
    second_half = floats[..., half_width:]
    turned = jnp.concatenate(
        [
            first_half * cosine - second_half * sine_part,
            second_half * cosine + first_half * sine_part,
        ],
        axis=-1,
    )
    return turned.astype(jnp.bfloat16)


def rms_scaled(values, gain):
    floats = values.astype(jnp.float32)
    return floats * lax.rsqrt(jnp.mean(floats * floats, axis=-1, keepdims=True) + epsilon) * gain


def attend_kernel(heads_here, nope, channels, scale, me_ref, query_ref, shared_ref, ups_ref, out_ref):
    group = pl.program_id(0)
    columns = heads_here * nope
    me = me_ref[0]
    tokens = shared_ref.shape[1]
    ups = ups_ref[0].reshape(channels, 2 * columns)
    up_keys = ups[:, 0:columns]
    up_values = ups[:, columns : 2 * columns]
    up_values_t = jnp.transpose(up_values.astype(jnp.float32)).astype(jnp.bfloat16)

    def scores_of(chunk):
        latent = shared_ref[chunk, :, 0:channels]
        turned = shared_ref[chunk, :, channels:]
        keys = jnp.dot(latent, up_keys, preferred_element_type=jnp.float32).astype(jnp.bfloat16)
        values_t = lax.dot_general(
            up_values_t, latent, (((1,), (1,)), ((), ())), preferred_element_type=jnp.float32
        ).astype(jnp.bfloat16)
        scores = []
        for head in range(heads_here):
            full = jnp.concatenate([keys[:, head * nope : (head + 1) * nope], turned], axis=1)
            scores.append(
                jnp.dot(full, query_ref[head], preferred_element_type=jnp.float32)
                * (scale * log2_e)
            )
        return scores, [values_t[h * nope : (h + 1) * nope, :] for h in range(heads_here)]

    key_ids = lax.broadcasted_iota(jnp.int32, (tokens, tokens), 0)
    query_ids = lax.broadcasted_iota(jnp.int32, (tokens, tokens), 1)
    allowed = key_ids <= query_ids
    scores, values = scores_of(me)
    state = []
    for score, value in zip(scores, values):
        score = jnp.where(allowed, score, masked_score)
        largest = jnp.max(score, axis=0, keepdims=True)
        powers = jnp.exp2(score - largest)
        state.append(
            (
                largest,
                jnp.sum(powers, axis=0, keepdims=True),
                jnp.dot(value, powers.astype(jnp.bfloat16), preferred_element_type=jnp.float32),
            )
        )

    def step(chunk, state):
        scores, values = scores_of(chunk)
        after = []
        for (largest, total, kept), score, value in zip(state, scores, values):
            now = jnp.maximum(largest, jnp.max(score, axis=0, keepdims=True))
            fade = jnp.exp2(largest - now)
            powers = jnp.exp2(score - now)
            after.append(
                (
                    now,
                    total * fade + jnp.sum(powers, axis=0, keepdims=True),
                    kept * fade
                    + jnp.dot(
                        value, powers.astype(jnp.bfloat16), preferred_element_type=jnp.float32
                    ),
                )
            )
        return tuple(after)

    state = lax.fori_loop(0, me, step, tuple(state))
    for head, (_, total, kept) in enumerate(state):
        out_ref[:, head * nope : (head + 1) * nope] = jnp.transpose(kept / total).astype(
            out_ref.dtype
        )


def attend(me, queries_t, shared, ups, heads_here, nope, channels, scale):
    groups, tokens, width = shared.shape
    columns = heads_here * nope
    depth = queries_t.shape[1]
    return pl.pallas_call(
        functools.partial(attend_kernel, heads_here, nope, channels, scale),
        grid_spec=pltpu.PrefetchScalarGridSpec(
            num_scalar_prefetch=1,
            grid=(groups,),
            in_specs=[
                pl.BlockSpec((heads_here, depth, tokens), lambda g, me: (g, 0, 0)),
                pl.BlockSpec((groups, tokens, width), lambda g, me: (0, 0, 0)),
                pl.BlockSpec((1,) + ups.shape[1:], lambda g, me: (g, 0, 0, 0)),
            ],
            out_specs=pl.BlockSpec((tokens, columns), lambda g, me: (0, g)),
        ),
        out_shape=jax.ShapeDtypeStruct((tokens, groups * columns), jnp.bfloat16),
        cost_estimate=pl.CostEstimate(
            flops=20 * groups * tokens * groups * tokens * columns,
            bytes_accessed=2 * groups * tokens * width,
            transcendentals=0,
        ),
    )(me, queries_t, shared, ups)


def project_kernel(heads_ref, weight_ref, resid_ref, gain_ref, after_ref, normed_ref, square_ref):
    part = pl.program_id(0)
    rows, width = weight_ref.shape[0] * weight_ref.shape[2], weight_ref.shape[3]
    weight = weight_ref[...].reshape(rows, width)
    projected = (
        jnp.dot(heads_ref[...], weight, preferred_element_type=jnp.float32)
        .astype(jnp.bfloat16)
        .astype(jnp.float32)
    )
    after = resid_ref[...].astype(jnp.float32) + projected
    after_ref[part] = after

    @pl.when(part == 0)
    def _():
        square_ref[...] = jnp.zeros_like(square_ref)

    square_ref[...] += jnp.sum(after * after, axis=1, keepdims=True)

    @pl.when(part == pl.num_programs(0) - 1)
    def _():
        parts = after_ref.shape[0]
        factor = lax.rsqrt(square_ref[...] / (parts * width) + epsilon)
        for at in range(parts):
            cols = slice(at * width, (at + 1) * width)
            normed_ref[:, cols] = (after_ref[at] * factor * gain_ref[:, cols]).astype(
                normed_ref.dtype
            )


def project(heads, weights, resid, gain):
    groups, parts, rows, width = weights.shape
    tokens = heads.shape[0]
    return pl.pallas_call(
        project_kernel,
        grid=(parts,),
        in_specs=[
            pl.BlockSpec((tokens, groups * rows), lambda p: (0, 0)),
            pl.BlockSpec((groups, 1, rows, width), lambda p: (0, p, 0, 0)),
            pl.BlockSpec((tokens, width), lambda p: (0, p)),
            pl.BlockSpec((1, parts * width), lambda p: (0, 0)),
        ],
        out_specs=[
            pl.BlockSpec((parts, tokens, width), lambda p: (0, 0, 0)),
            pl.BlockSpec((tokens, parts * width), lambda p: (0, 0)),
        ],
        out_shape=[
            jax.ShapeDtypeStruct((parts, tokens, width), jnp.float32),
            jax.ShapeDtypeStruct((tokens, parts * width), jnp.bfloat16),
        ],
        scratch_shapes=[pltpu.VMEM((tokens, 1), jnp.float32)],
        cost_estimate=pl.CostEstimate(
            flops=2 * tokens * groups * rows * parts * width,
            bytes_accessed=2 * groups * rows * parts * width,
            transcendentals=0,
        ),
    )(heads, weights, resid, gain)


def in_three(values):
    high = lax.reduce_precision(values, 8, 7)
    middle = lax.reduce_precision(values - high, 8, 7)
    low = values - high - middle
    return [piece.astype(jnp.bfloat16) for piece in (high, middle, low)]


def shards(
    query_nope,
    query_rope,
    latent,
    key_rope,
    resid,
    latent_gain,
    key_up,
    value_up,
    out_proj,
    norm_gain,
    expert_gate,
    expert_up,
    expert_down,
    routes,
    route_weight,
):
    tokens, channels = latent.shape[1:]
    sp_count = lax.axis_size("sp")
    dp_count = lax.axis_size("dp")
    me = lax.axis_index("sp")
    nope, rope = query_nope.shape[-1], query_rope.shape[-1]
    heads_here = key_up.shape[1] // nope
    scale = (nope + rope) ** (-0.5)
    local_pos = me * tokens + jnp.arange(tokens, dtype=jnp.int32)
    latent_normed = rms_scaled(latent[0], latent_gain).astype(jnp.bfloat16)
    key_turned = rotate(key_rope[0], local_pos)
    spare = 128 - rope
    shared = lax.all_gather(
        jnp.concatenate(
            [latent_normed, key_turned, jnp.zeros((tokens, spare), jnp.bfloat16)],
            axis=1,
        ),
        "sp",
        axis=0,
    )
    piece = channels // dp_count
    ups = lax.dynamic_slice_in_dim(
        jnp.concatenate([key_up, value_up], axis=1), lax.axis_index("dp") * piece, piece, axis=0
    )
    ups = lax.all_gather(ups, ("sp", "dp"), axis=0).reshape(sp_count, dp_count, piece, -1)
    weights = lax.all_gather(out_proj, ("sp", "dp"), axis=0)
    weights = weights.reshape(sp_count, dp_count, *out_proj.shape)
    query_turned = rotate(query_rope[0], local_pos)
    queries = jnp.concatenate(
        [query_nope[0], query_turned, jnp.zeros(query_turned.shape[:2] + (128 - rope,), jnp.bfloat16)],
        axis=-1,
    )
    queries_t = jnp.transpose(queries, (1, 2, 0))
    heads = attend(
        me.astype(jnp.int32)[None], queries_t, shared, ups, heads_here, nope, channels, scale
    )
    after, normed = project(heads, weights, resid[0], norm_gain[None])

    experts_all = sp_count * expert_gate.shape[0]
    capacity = 4 * tokens // experts_all
    ids = jnp.arange(experts_all, dtype=jnp.int32)[:, None, None]
    mine = routes[0][None] == ids
    named = jnp.any(mine, axis=-1)
    weight = jnp.sum(jnp.where(mine, route_weight[0][None], 0.0), axis=-1)
    place = jnp.cumsum(named.astype(jnp.int32), axis=1) - 1
    chosen = (
        place[:, None, :] == jnp.arange(capacity, dtype=jnp.int32)[None, :, None]
    ) & named[:, None, :]
    select = chosen.astype(jnp.bfloat16).reshape(experts_all * capacity, tokens)
    outgoing = jnp.dot(select, normed, preferred_element_type=jnp.float32).astype(jnp.bfloat16)
    rows = lax.all_to_all(outgoing, "sp", split_axis=0, concat_axis=0, tiled=True)
    gate = jnp.dot(rows, expert_gate[0], preferred_element_type=jnp.float32)
    upward = jnp.dot(rows, expert_up[0], preferred_element_type=jnp.float32)
    hidden = (jax.nn.silu(gate) * upward).astype(jnp.bfloat16)
    result = jnp.dot(hidden, expert_down[0], preferred_element_type=jnp.float32).astype(
        jnp.bfloat16
    )
    returned = lax.all_to_all(result, "sp", split_axis=0, concat_axis=0, tiled=True)
    mixing = jnp.where(chosen, weight[:, None, :], 0.0).reshape(experts_all * capacity, tokens)
    routed = sum(
        lax.dot_general(part, returned, (((0,), (0,)), ((), ())), preferred_element_type=jnp.float32)
        for part in in_three(mixing)[0:2]
    )
    after = jnp.concatenate([after[p] for p in range(dp_count)], axis=1)
    return (after + routed).astype(jnp.bfloat16)[None]


def solution(mesh):
    return jax.shard_map(
        shards,
        mesh=mesh,
        in_specs=(
            P("dp", "sp", None, None),
            P("dp", "sp", None, None),
            P("dp", "sp", None),
            P("dp", "sp", None),
            P("dp", "sp", None),
            P(),
            P(None, "sp"),
            P(None, "sp"),
            P("sp", "dp"),
            P(),
            P("sp", None, None),
            P("sp", None, None),
            P("sp", None, None),
            P("dp", "sp", None),
            P("dp", "sp", None),
        ),
        out_specs=P("dp", "sp", None),
        check_vma=False,
    )
```

```python
import functools
import math

import jax
import jax.numpy as jnp
from jax import lax
from jax.experimental import pallas as pl
from jax.experimental.pallas import tpu as pltpu
from jax.sharding import PartitionSpec as P

epsilon = 1e-06
rope_base = 10000.0
masked_score = -1e30
log2_e = 1.4426950408889634


def rotate(values, positions):
    half_width = values.shape[-1] // 2
    frequency = rope_base ** (-jnp.arange(half_width, dtype=jnp.float32) / half_width)
    angles = positions.astype(jnp.float32)[:, None] * frequency[None, :]
    cosine = jnp.cos(angles)
    sine_part = jnp.sin(angles)
    if values.ndim == 3:
        cosine = cosine[:, None, :]
        sine_part = sine_part[:, None, :]
    floats = values.astype(jnp.float32)
    first_half = floats[..., :half_width]
    second_half = floats[..., half_width:]
    turned = jnp.concatenate(
        [
            first_half * cosine - second_half * sine_part,
            second_half * cosine + first_half * sine_part,
        ],
        axis=-1,
    )
    return turned.astype(jnp.bfloat16)


def rms_scaled(values, gain):
    floats = values.astype(jnp.float32)
    return floats * lax.rsqrt(jnp.mean(floats * floats, axis=-1, keepdims=True) + epsilon) * gain


def attend_kernel(heads_here, nope, channels, scale, me_ref, query_ref, shared_ref, ups_ref, out_ref):
    group = pl.program_id(0)
    columns = heads_here * nope
    me = me_ref[0]
    tokens = shared_ref.shape[1]
    ups = ups_ref[...].reshape(channels, 2 * columns)
    up_keys = ups[:, 0:columns]
    up_values = ups[:, columns : 2 * columns]
    up_values_t = jnp.transpose(up_values.astype(jnp.float32)).astype(jnp.bfloat16)

    def scores_of(chunk):
        latent = shared_ref[chunk, :, 0:channels]
        turned = shared_ref[chunk, :, channels:]
        keys = jnp.dot(latent, up_keys, preferred_element_type=jnp.float32).astype(jnp.bfloat16)
        values_t = lax.dot_general(
            up_values_t, latent, (((1,), (1,)), ((), ())), preferred_element_type=jnp.float32
        ).astype(jnp.bfloat16)
        scores = []
        for head in range(heads_here):
            full = jnp.concatenate([keys[:, head * nope : (head + 1) * nope], turned], axis=1)
            scores.append(
                jnp.dot(full, query_ref[head], preferred_element_type=jnp.float32)
                * (scale * log2_e)
            )
        return scores, [values_t[h * nope : (h + 1) * nope, :] for h in range(heads_here)]

    key_ids = lax.broadcasted_iota(jnp.int32, (tokens, tokens), 0)
    query_ids = lax.broadcasted_iota(jnp.int32, (tokens, tokens), 1)
    allowed = key_ids <= query_ids
    scores, values = scores_of(me)
    state = []
    for score, value in zip(scores, values):
        score = jnp.where(allowed, score, masked_score)
        largest = jnp.max(score, axis=0, keepdims=True)
        powers = jnp.exp2(score - largest)
        state.append(
            (
                largest,
                jnp.sum(powers, axis=0, keepdims=True),
                jnp.dot(value, powers.astype(jnp.bfloat16), preferred_element_type=jnp.float32),
            )
        )

    def step(chunk, state):
        scores, values = scores_of(chunk)
        after = []
        for (largest, total, kept), score, value in zip(state, scores, values):
            now = jnp.maximum(largest, jnp.max(score, axis=0, keepdims=True))
            fade = jnp.exp2(largest - now)
            powers = jnp.exp2(score - now)
            after.append(
                (
                    now,
                    total * fade + jnp.sum(powers, axis=0, keepdims=True),
                    kept * fade
                    + jnp.dot(
                        value, powers.astype(jnp.bfloat16), preferred_element_type=jnp.float32
                    ),
                )
            )
        return tuple(after)

    state = lax.fori_loop(0, me, step, tuple(state))
    for head, (_, total, kept) in enumerate(state):
        out_ref[:, head * nope : (head + 1) * nope] = jnp.transpose(kept / total).astype(
            out_ref.dtype
        )


def attend(me, queries_t, shared, ups, heads_here, nope, channels, scale):
    groups, tokens, width = shared.shape
    columns = heads_here * nope
    depth = queries_t.shape[1]
    return pl.pallas_call(
        functools.partial(attend_kernel, heads_here, nope, channels, scale),
        grid_spec=pltpu.PrefetchScalarGridSpec(
            num_scalar_prefetch=1,
            grid=(groups,),
            in_specs=[
                pl.BlockSpec((heads_here, depth, tokens), lambda g, me: (g, 0, 0)),
                pl.BlockSpec((groups, tokens, width), lambda g, me: (0, 0, 0)),
                pl.BlockSpec((ups.shape[0], 1) + ups.shape[2:], lambda g, me: (0, g, 0, 0)),
            ],
            out_specs=pl.BlockSpec((tokens, columns), lambda g, me: (0, g)),
        ),
        out_shape=jax.ShapeDtypeStruct((tokens, groups * columns), jnp.bfloat16),
        cost_estimate=pl.CostEstimate(
            flops=20 * groups * tokens * groups * tokens * columns,
            bytes_accessed=2 * groups * tokens * width,
            transcendentals=0,
        ),
    )(me, queries_t, shared, ups)


def project_kernel(heads_ref, weight_ref, resid_ref, gain_ref, after_ref, normed_ref, square_ref):
    part = pl.program_id(0)
    rows, width = weight_ref.shape[0] * weight_ref.shape[2], weight_ref.shape[3]
    weight = weight_ref[...].reshape(rows, width)
    projected = (
        jnp.dot(heads_ref[...], weight, preferred_element_type=jnp.float32)
        .astype(jnp.bfloat16)
        .astype(jnp.float32)
    )
    after = resid_ref[...].astype(jnp.float32) + projected
    after_ref[part] = after

    @pl.when(part == 0)
    def _():
        square_ref[...] = jnp.zeros_like(square_ref)

    square_ref[...] += jnp.sum(after * after, axis=1, keepdims=True)

    @pl.when(part == pl.num_programs(0) - 1)
    def _():
        parts = after_ref.shape[0]
        factor = lax.rsqrt(square_ref[...] / (parts * width) + epsilon)
        for at in range(parts):
            cols = slice(at * width, (at + 1) * width)
            normed_ref[:, cols] = (after_ref[at] * factor * gain_ref[:, cols]).astype(
                normed_ref.dtype
            )


def project(heads, weights, resid, gain):
    groups, parts, rows, width = weights.shape
    tokens = heads.shape[0]
    return pl.pallas_call(
        project_kernel,
        grid=(parts,),
        in_specs=[
            pl.BlockSpec((tokens, groups * rows), lambda p: (0, 0)),
            pl.BlockSpec((groups, 1, rows, width), lambda p: (0, p, 0, 0)),
            pl.BlockSpec((tokens, width), lambda p: (0, p)),
            pl.BlockSpec((1, parts * width), lambda p: (0, 0)),
        ],
        out_specs=[
            pl.BlockSpec((parts, tokens, width), lambda p: (0, 0, 0)),
            pl.BlockSpec((tokens, parts * width), lambda p: (0, 0)),
        ],
        out_shape=[
            jax.ShapeDtypeStruct((parts, tokens, width), jnp.float32),
            jax.ShapeDtypeStruct((tokens, parts * width), jnp.bfloat16),
        ],
        scratch_shapes=[pltpu.VMEM((tokens, 1), jnp.float32)],
        cost_estimate=pl.CostEstimate(
            flops=2 * tokens * groups * rows * parts * width,
            bytes_accessed=2 * groups * rows * parts * width,
            transcendentals=0,
        ),
    )(heads, weights, resid, gain)


def gather_kernel(
    outer, inner, dp_count, row_ref, piece_ref, rows_ref, pieces_ref,
    own_sems, far_send, far_recv, near_send, near_recv, dp_send, dp_recv,
):
    me = lax.axis_index("sp")
    dp = lax.axis_index("dp")
    far, near = me // inner, lax.rem(me, inner)
    barrier = pltpu.get_barrier_semaphore()
    fars = [lax.rem(far + step, outer) for step in range(1, outer)]
    nears = [lax.rem(near + step, inner) for step in range(1, inner)]
    dps = [lax.rem(dp + step, dp_count) for step in range(1, dp_count)]
    greeted = (
        [{"sp": f * inner + near} for f in fars]
        + [{"sp": far * inner + n} for n in nears]
        + [{"dp": d} for d in dps]
    )
    for peer in greeted:
        pl.semaphore_signal(barrier, inc=1, device_id=peer, device_id_type=pl.DeviceIdType.MESH)
    pl.semaphore_wait(barrier, len(greeted))

    def remote(source, target, send, recv, peer):
        copy = pltpu.make_async_remote_copy(
            src_ref=source, dst_ref=target, send_sem=send, recv_sem=recv,
            device_id=peer, device_id_type=pl.DeviceIdType.MESH,
        )
        copy.start()
        return copy

    def pair(row, piece, block, send, recv, peer):
        return [
            remote(row, rows_ref.at[block], send.at[0], recv.at[0], peer),
            remote(piece, pieces_ref.at[dp, block], send.at[1], recv.at[1], peer),
        ]

    out_far = []
    for at, f in enumerate(fars):
        out_far.append(pair(row_ref, piece_ref, me, far_send.at[at], far_recv.at[at], {"sp": f * inner + near}))
    last = []

    def share(block):
        for at, d in enumerate(dps):
            last.append(
                remote(
                    pieces_ref.at[dp, block], pieces_ref.at[dp, block],
                    dp_send.at[len(last)], dp_recv.at[len(last)], {"dp": d},
                )
            )

    sends = []
    for at, n in enumerate(nears):
        sends.append(pair(row_ref, piece_ref, me, near_send.at[0, at], near_recv.at[0, at], {"sp": far * inner + n}))
    own = [
        pltpu.make_async_copy(row_ref, rows_ref.at[me], own_sems.at[0]),
        pltpu.make_async_copy(piece_ref, pieces_ref.at[dp, me], own_sems.at[1]),
    ]
    for copy in own:
        copy.start()
    for copy in own:
        copy.wait()
    share(me)
    for at in range(outer - 1):
        for copy in out_far[at]:
            copy.wait_recv()
        block = lax.rem(far + outer - 1 - at, outer) * inner + near
        for to, n in enumerate(nears):
            sends.append(
                pair(
                    rows_ref.at[block], pieces_ref.at[dp, block], block,
                    near_send.at[at + 1, to], near_recv.at[at + 1, to], {"sp": far * inner + n},
                )
            )
        share(block)
    for at in range(outer):
        for to in range(inner - 1):
            for copy in sends[at * (inner - 1) + to]:
                copy.wait_recv()
            column = lax.rem(near + inner - 1 - to, inner)
            share(lax.rem(far + outer - at, outer) * inner + column)
    for copies in out_far + sends:
        for copy in copies:
            copy.wait_send()
    for copy in last:
        copy.wait()


def gather_shared(row, piece, sp_count, dp_count, number):
    inner = max(d for d in range(1, math.isqrt(sp_count) + 1) if sp_count % d == 0)
    outer = sp_count // inner
    dma = pltpu.SemaphoreType.DMA
    return pl.pallas_call(
        functools.partial(gather_kernel, outer, inner, dp_count),
        out_shape=[
            jax.ShapeDtypeStruct((sp_count,) + row.shape, row.dtype),
            jax.ShapeDtypeStruct((dp_count, sp_count) + piece.shape, piece.dtype),
        ],
        in_specs=[pl.BlockSpec(memory_space=pltpu.VMEM)] * 2,
        out_specs=[pl.BlockSpec(memory_space=pltpu.VMEM)] * 2,
        scratch_shapes=[
            dma((2,)),
            dma((max(outer - 1, 1), 2)),
            dma((max(outer - 1, 1), 2)),
            dma((outer, max(inner - 1, 1), 2)),
            dma((outer, max(inner - 1, 1), 2)),
            dma((max(dp_count - 1, 1) * sp_count,)),
            dma((max(dp_count - 1, 1) * sp_count,)),
        ],
        compiler_params=pltpu.CompilerParams(collective_id=number, has_side_effects=True),
        cost_estimate=pl.CostEstimate(flops=2 * 10**10, bytes_accessed=10**7, transcendentals=0),
    )(row, piece)


def in_three(values):
    high = lax.reduce_precision(values, 8, 7)
    middle = lax.reduce_precision(values - high, 8, 7)
    low = values - high - middle
    return [piece.astype(jnp.bfloat16) for piece in (high, middle, low)]


def shards(
    query_nope,
    query_rope,
    latent,
    key_rope,
    resid,
    latent_gain,
    key_up,
    value_up,
    out_proj,
    norm_gain,
    expert_gate,
    expert_up,
    expert_down,
    routes,
    route_weight,
):
    tokens, channels = latent.shape[1:]
    sp_count = lax.axis_size("sp")
    dp_count = lax.axis_size("dp")
    me = lax.axis_index("sp")
    nope, rope = query_nope.shape[-1], query_rope.shape[-1]
    heads_here = key_up.shape[1] // nope
    scale = (nope + rope) ** (-0.5)
    local_pos = me * tokens + jnp.arange(tokens, dtype=jnp.int32)
    latent_normed = rms_scaled(latent[0], latent_gain).astype(jnp.bfloat16)
    key_turned = rotate(key_rope[0], local_pos)
    spare = 128 - rope
    row = jnp.concatenate(
        [latent_normed, key_turned, jnp.zeros((tokens, spare), jnp.bfloat16)], axis=1
    )
    piece = channels // dp_count
    ups = lax.dynamic_slice_in_dim(
        jnp.concatenate([key_up, value_up], axis=1), lax.axis_index("dp") * piece, piece, axis=0
    )
    shared, ups = gather_shared(row, ups, sp_count, dp_count, 0)
    weights = lax.all_gather(out_proj, ("sp", "dp"), axis=0)
    weights = weights.reshape(sp_count, dp_count, *out_proj.shape)
    query_turned = rotate(query_rope[0], local_pos)
    queries = jnp.concatenate(
        [query_nope[0], query_turned, jnp.zeros(query_turned.shape[:2] + (128 - rope,), jnp.bfloat16)],
        axis=-1,
    )
    queries_t = jnp.transpose(queries, (1, 2, 0))
    heads = attend(
        me.astype(jnp.int32)[None], queries_t, shared, ups, heads_here, nope, channels, scale
    )
    after, normed = project(heads, weights, resid[0], norm_gain[None])

    experts_all = sp_count * expert_gate.shape[0]
    capacity = 4 * tokens // experts_all
    ids = jnp.arange(experts_all, dtype=jnp.int32)[:, None, None]
    mine = routes[0][None] == ids
    named = jnp.any(mine, axis=-1)
    weight = jnp.sum(jnp.where(mine, route_weight[0][None], 0.0), axis=-1)
    place = jnp.cumsum(named.astype(jnp.int32), axis=1) - 1
    chosen = (
        place[:, None, :] == jnp.arange(capacity, dtype=jnp.int32)[None, :, None]
    ) & named[:, None, :]
    select = chosen.astype(jnp.bfloat16).reshape(experts_all * capacity, tokens)
    outgoing = jnp.dot(select, normed, preferred_element_type=jnp.float32).astype(jnp.bfloat16)
    rows = lax.all_to_all(outgoing, "sp", split_axis=0, concat_axis=0, tiled=True)
    gate = jnp.dot(rows, expert_gate[0], preferred_element_type=jnp.float32)
    upward = jnp.dot(rows, expert_up[0], preferred_element_type=jnp.float32)
    hidden = (jax.nn.silu(gate) * upward).astype(jnp.bfloat16)
    result = jnp.dot(hidden, expert_down[0], preferred_element_type=jnp.float32).astype(
        jnp.bfloat16
    )
    returned = lax.all_to_all(result, "sp", split_axis=0, concat_axis=0, tiled=True)
    mixing = jnp.where(chosen, weight[:, None, :], 0.0).reshape(experts_all * capacity, tokens)
    routed = sum(
        lax.dot_general(part, returned, (((0,), (0,)), ((), ())), preferred_element_type=jnp.float32)
        for part in in_three(mixing)[0:2]
    )
    after = jnp.concatenate([after[p] for p in range(dp_count)], axis=1)
    return (after + routed).astype(jnp.bfloat16)[None]


def solution(mesh):
    return jax.shard_map(
        shards,
        mesh=mesh,
        in_specs=(
            P("dp", "sp", None, None),
            P("dp", "sp", None, None),
            P("dp", "sp", None),
            P("dp", "sp", None),
            P("dp", "sp", None),
            P(),
            P(None, "sp"),
            P(None, "sp"),
            P("sp", "dp"),
            P(),
            P("sp", None, None),
            P("sp", None, None),
            P("sp", None, None),
            P("dp", "sp", None),
            P("dp", "sp", None),
        ),
        out_specs=P("dp", "sp", None),
        check_vma=False,
    )
```
